32 devices in a mesh: dp: 4 (over y, x), kv: 4 (over z), tp: 2 (over core).
Axes of the slice: x: 2, y: 2, z: 4, core: 2. Of those that a mesh axis runs over, the one named last changes fastest.
Arguments:
- tokens: bfloat16 [64, 4096], P('dp', 'kv'), may hold values from -51 to 51
- norm_gain: float32 [4096], P('kv'), may hold values from 0.1 to 1.9
- w_query: bfloat16 [4096, 2048], P('kv', 'tp'), may hold values from -0.09375 to 0.09375
- lambda_head: float32 [16], P('tp'), may hold values from 0.3 to 0.8
- head_gain: float32 [128], replicated, may hold values from 0.1 to 1.9
- w_out: bfloat16 [2048, 4096], P('tp', 'kv'), may hold values from -0.125 to 0.125
- rotated_key_cache: bfloat16 [64, 1024, 128], P('dp', 'kv'), may hold values from -540 to 540, as said below
- value_cache: bfloat16 [64, 1024, 128], P('dp', 'kv'), may hold values from -6 to 6
- lengths: int32 [64], P('dp'), may hold values from 256 to 1024
Outputs:
- mixed: bfloat16 [64, 4096], P('dp', ('kv', 'tp'))
The draws below stay inside these ranges and needn't reach their ends.
Inputs may be any that keep to these rules, and one draw needn't show every extreme that they name: `rotated_key_cache`: keys have an order-one typical size. The new token is the last filled position, lengths - 1.
All inputs are finite; a program needn't handle non-finite values.
Results may differ from the reference program's by a relative error of at most 0.0112.
Values may be sent and summed in bfloat16 or wider, within the bound.
No kernel may reach another device: no remote copies, remote signals or barrier semaphores. Data moves between devices by JAX's collectives and lax.ppermute only.
A program may use at most 64 MiB of HBM per device.

```python
import jax
import jax.numpy as jnp
from jax import lax

D = 4096
HEADS = 16
HEAD_FEATURES = 64
VALUE_DIM = 128
SEQS = 64
CTX = 1024


def draw_tokens(key, part):
    column_scaling = jnp.exp(jnp.log(3.0) * jnp.arange(D, dtype=jnp.float32) / D)
    base = jnp.clip(jax.random.normal(key, (SEQS, D), jnp.float32), -6.0, 6.0)
    values = base * column_scaling[None, :]
    return values.astype(jnp.bfloat16)


def draw_rotated_key_cache(key, part):
    base = jnp.clip(jax.random.normal(key, (SEQS, CTX, 2 * HEAD_FEATURES), jnp.float32), -5.0, 5.0) * 1.8
    return base.astype(jnp.bfloat16)


def set_ends(values, own_key, smallest, largest):
    longest = values.shape.index(max(values.shape))
    spots = []
    for shift in (0, 1):
        where = [jax.random.randint(jax.random.fold_in(own_key, axis), (), 0, length) for axis, length in enumerate(values.shape)]
        where[longest] = (where[longest] + shift) % values.shape[longest]
        spots.append(tuple(where))
    return values.at[spots[0]].set(smallest).at[spots[1]].set(largest)


def block_scale(stream_key, extent, pieces, least, largest):
    level, own = 1.0, jax.random.fold_in(stream_key, 6)
    for dim, blocks in pieces:
        heights = jnp.exp(jax.random.uniform(jax.random.fold_in(own, dim), (blocks,), jnp.float32, least / len(pieces), largest / len(pieces)))
        level = level * jnp.repeat(heights, extent[dim] // blocks).reshape([-1 if axis == dim else 1 for axis in range(len(extent))])
    return level


def noise(key, shape, spread, most, shards=(), kind=jnp.bfloat16):
    values = spread * jax.random.normal(key, shape, jnp.float32)
    if shards:
        values = values * block_scale(key, shape, shards, -0.22, 0.18)
    return jnp.clip(values, -most, most).astype(kind)


def setup_inputs(seed: int = 0) -> dict:
    splits = jax.random.split(jax.random.key(seed), 10)
    return {
        "tokens": draw_tokens(jax.random.fold_in(splits[9], 71), 0),
        "norm_gain": jnp.clip(1.0 + 0.18 * jax.random.normal(splits[1], (D,), jnp.float32), 0.1, 1.9),
        "w_query": noise(splits[2], (D, HEADS * 2 * HEAD_FEATURES), D ** -0.5, 0.09375, ((0, 4), (1, 2))),
        "lambda_head": jnp.clip(0.3 + 0.5 * jax.random.uniform(splits[3], (HEADS,), jnp.float32) ** block_scale(splits[3], (HEADS,), ((0, 2),), -0.2, 0.2), 0.3, 0.8),
        "head_gain": jnp.clip(1.0 + 0.18 * jax.random.normal(splits[4], (VALUE_DIM,), jnp.float32), 0.1, 1.9),
        "w_out": noise(splits[5], (HEADS * VALUE_DIM, D), (HEADS * VALUE_DIM) ** -0.5, 0.125, ((0, 2), (1, 4))),
        "rotated_key_cache": draw_rotated_key_cache(jax.random.fold_in(splits[9], 71), 0),
        "value_cache": noise(splits[7], (SEQS, CTX, VALUE_DIM), 1.0, 6.0, ((0, 4), (1, 4))),
        "lengths": set_ends(jax.random.randint(splits[8], (SEQS,), CTX // 4, CTX + 1), jax.random.fold_in(splits[8], 1), CTX // 4, CTX).astype(jnp.int32),
    }


EPS = 1e-05

def rotate_query(query, position):
    half_dim = query.shape[-1] // 2
    frequency = 1.0 / 10000.0 ** (jnp.arange(half_dim, dtype=jnp.float32) / half_dim)
    angles = position[:, None] * frequency[None, :]
    cosine_table = jnp.concatenate([jnp.cos(angles), jnp.cos(angles)], -1)[:, None, None, :]
    sine_table = jnp.concatenate([jnp.sin(angles), jnp.sin(angles)], -1)[:, None, None, :]
    first_half = query[..., :half_dim]
    second_half = query[..., half_dim:]
    turned = jnp.concatenate([-second_half, first_half], -1)
    return query * cosine_table + turned * sine_table

def finish(numerators, totals, lambdas, head_gain):
    averaged = numerators / totals[..., None]
    head_result = averaged[..., 0, :] - lambdas[..., None] * averaged[..., 1, :]
    factor = lax.rsqrt(lax.optimization_barrier(jnp.mean(head_result * head_result, -1, keepdims=True)) + EPS)
    return (head_result * factor * head_gain).astype(jnp.bfloat16)

def reference(tokens, norm_gain, w_query, lambda_head, head_gain, w_out, rotated_key_cache, value_cache, lengths):
    widened = tokens.astype(jnp.float32)
    squares = lax.optimization_barrier(jnp.sum(widened * widened, -1))
    scale_rows = lax.rsqrt(squares / D + EPS)
    scaled_in = (widened * norm_gain).astype(jnp.bfloat16)
    raw_query = jnp.dot(scaled_in, w_query, preferred_element_type=jnp.float32)
    shaped = (raw_query * scale_rows[:, None]).reshape(SEQS, HEADS, 2, HEAD_FEATURES)
    query = rotate_query(shaped, (lengths - 1).astype(jnp.float32))

    def one_sequence(items):
        query_vector, keys, values, length = items
        keys_sidebyside = keys.astype(jnp.float32).reshape(CTX, 2, HEAD_FEATURES)
        score_rows = jnp.einsum('lxi,wxi->lxw', query_vector, keys_sidebyside, precision=lax.Precision.HIGHEST) * HEAD_FEATURES ** (-0.5)
        valid = jnp.arange(CTX, dtype=jnp.int32) < length
        masked = jnp.where(valid, score_rows, -1e+30)
        maxima = lax.optimization_barrier(jnp.max(masked, -1, keepdims=True))
        weights = jnp.where(valid, jnp.exp(masked - maxima), 0.0)
        totals = lax.optimization_barrier(jnp.sum(weights, -1))
        rounded = lax.optimization_barrier(weights.astype(jnp.bfloat16)).astype(jnp.float32)
        numerators = jnp.einsum('hmp,pv->hmv', rounded, values.astype(jnp.float32))
        return (numerators, totals)
    numerators, totals = lax.map(one_sequence, (query, rotated_key_cache, value_cache, lengths))
    normed = finish(numerators, totals, lambda_head[None, :], head_gain)
    flat = normed.reshape(SEQS, HEADS * VALUE_DIM)
    return jnp.dot(flat, w_out, preferred_element_type=jnp.float32).astype(jnp.bfloat16)
```

```python
import functools

import jax
import jax.numpy as jnp
from jax import lax
from jax.experimental import pallas as pl
from jax.experimental.pallas import tpu as pltpu
from jax.sharding import PartitionSpec as P


HEAD_FEATURES = 64
VALUE_DIM = 128
LANES = 128
EPS = 1e-05
ROPE_BASE = 10000.0
MASKED = -1e30
F32 = jnp.float32
BF16 = jnp.bfloat16
VMEM = pl.BlockSpec(memory_space=pltpu.VMEM)
SMEM = pl.BlockSpec(memory_space=pltpu.SMEM)


def lane_index(shape):
    return lax.broadcasted_iota(jnp.int32, shape, len(shape) - 1)


def split3(x):
    high = x.astype(BF16).astype(F32)
    rest = x - high
    middle = rest.astype(BF16).astype(F32)
    return high, middle, (rest - middle).astype(BF16).astype(F32)


def project_kernel(tokens_ref, gain_ref, weights_ref, out_ref):
    heads = out_ref.shape[0] - 1
    widened = tokens_ref[...].astype(F32)
    squares = jnp.sum(widened * widened, -1, keepdims=True)
    scaled = (widened * gain_ref[...]).astype(BF16)
    part = jnp.dot(scaled, weights_ref[...], preferred_element_type=F32)
    for head in range(heads):
        out_ref[head] = part[:, head * LANES : (head + 1) * LANES]
    out_ref[heads] = jnp.broadcast_to(squares, out_ref.shape[1:])


def attend_kernel(width, count, limits_ref, *refs):
    parts, (cosine_ref, sine_ref, keys_ref, values_ref, out_ref, query_ref) = refs[:count], refs[count:]
    heads = parts[0].shape[0] - 1
    seqs, positions = keys_ref.shape[:2]

    def summed(index):
        total = parts[0][index]
        for part in parts[1:]:
            total = total + part[index]
        return total

    scale = lax.rsqrt(summed(heads) / width + EPS) * HEAD_FEATURES ** (-0.5)
    cosine, sine = cosine_ref[...] * scale, sine_ref[...] * scale
    half = HEAD_FEATURES // 2
    low = (lane_index(cosine.shape) % HEAD_FEATURES) < half
    for head in range(heads):
        raw = summed(head)
        turned = jnp.where(low, pltpu.roll(raw, LANES - half, 1), pltpu.roll(raw, half, 1))
        query_ref[:, head, :] = raw * cosine + turned * sine

    first = lane_index((heads, LANES)) < HEAD_FEATURES
    rows = 2 * heads
    lanes = lane_index((rows, LANES))
    places = lane_index((rows, positions))
    maxima = jnp.zeros((rows, LANES), F32)
    totals = jnp.zeros((rows, LANES), F32)
    for seq in range(seqs):
        pieces = split3(query_ref[seq])
        left = jnp.concatenate(
            [jnp.where(keep, piece, 0.0) for piece in pieces for keep in (first, ~first)], 0
        ).astype(BF16)
        products = lax.dot_general(
            left, keys_ref[seq], (((1,), (1,)), ((), ())), preferred_element_type=F32
        )
        scores = products[:rows] + (products[rows : 2 * rows] + products[2 * rows :])
        valid = places < limits_ref[seq]
        masked = jnp.where(valid, scores, MASKED)
        top = jnp.max(masked, -1, keepdims=True)
        weights = jnp.where(valid, jnp.exp(masked - top), 0.0)
        maxima = jnp.where(lanes == seq, top, maxima)
        totals = jnp.where(lanes == seq, jnp.sum(weights, -1, keepdims=True), totals)
        out_ref[seq] = jnp.dot(
            weights.astype(BF16), values_ref[seq], preferred_element_type=F32
        ).astype(BF16)
    packed = jnp.zeros((rows, LANES), F32)
    for place, piece in enumerate(split3(maxima) + split3(totals)):
        inside = (lanes >= place * seqs) & (lanes < (place + 1) * seqs)
        moved = pltpu.roll(piece, place * seqs, 1) if place else piece
        packed = jnp.where(inside, moved, packed)
    out_ref[seqs] = packed.astype(BF16)


def combine(parts, signs_ref, gain_ref, mixed_ref):
    seqs, rows = parts[0].shape[0] - 1, parts[0].shape[1]
    heads = rows // 2

    def unpacked(part, place):
        packed = part[seqs].astype(F32)
        total = None
        for piece in range(place, place + 3):
            moved = pltpu.roll(packed, LANES - piece * seqs, 1) if piece else packed
            total = moved if total is None else total + moved
        return total

    maxima = [unpacked(part, 0) for part in parts]
    top = functools.reduce(jnp.maximum, maxima)
    factors = [jnp.exp(own - top) for own in maxima]
    totals = sum(factor * unpacked(part, 3) for factor, part in zip(factors, parts))
    shares = signs_ref[...] / totals
    factors = [factor * shares for factor in factors]
    gain = gain_ref[...]
    for seq in range(seqs):
        both = sum(
            factor[:, seq : seq + 1] * part[seq].astype(F32) for factor, part in zip(factors, parts)
        )
        head_out = both[:heads] + both[heads:]
        mean = jnp.mean(head_out * head_out, -1, keepdims=True)
        mixed_ref[seq] = head_out * lax.rsqrt(mean + EPS) * gain


def finish_kernel(count, side_ref, *refs):
    parts = refs[:count]
    signs_ref, gain_ref, weights_ref, normed_ref, sent_ref, mixed_ref = refs[count:]
    combine(parts, signs_ref, gain_ref, mixed_ref)
    for head in range(mixed_ref.shape[1]):
        normed_ref[:, head * VALUE_DIM : (head + 1) * VALUE_DIM] = mixed_ref[:, head, :].astype(BF16)
    width = sent_ref.shape[1]
    start = pl.multiple_of((1 - side_ref[0]) * width, width)
    sent_ref[...] = jnp.dot(
        normed_ref[...], weights_ref[:, pl.ds(start, width)], preferred_element_type=F32
    )


def own_kernel(side_ref, normed_ref, weights_ref, out_ref):
    width = out_ref.shape[1]
    start = pl.multiple_of(side_ref[0] * width, width)
    out_ref[...] = jnp.dot(
        normed_ref[...], weights_ref[:, pl.ds(start, width)], preferred_element_type=F32
    )


def call(kernel, out_shape, in_specs, scratch=(), flops=0):
    out_specs = jax.tree.map(lambda _: VMEM, out_shape)
    return pl.pallas_call(
        kernel,
        out_shape=out_shape,
        in_specs=in_specs,
        out_specs=out_specs,
        scratch_shapes=scratch,
        cost_estimate=pl.CostEstimate(flops=flops, bytes_accessed=1 << 20, transcendentals=0),
    )


def exchanged(x, axis):
    count = lax.axis_size(axis)
    received = []
    for step in range(count - 1, 0, -1):
        pairs = [(source, source ^ step) for source in range(count)]
        received.append(lax.ppermute(x, axis, pairs))
    return [x] + received


def tables(lengths, copies):
    half = HEAD_FEATURES // 2
    frequency = 1.0 / ROPE_BASE ** (jnp.arange(half, dtype=F32) / half)
    angles = (lengths - 1).astype(F32)[:, None] * frequency[None, :]
    cosine, sine = jnp.cos(angles), jnp.sin(angles)
    return (
        jnp.concatenate([cosine, cosine] * copies, -1),
        jnp.concatenate([-sine, sine] * copies, -1),
    )


def near_device(
    tokens, norm_gain, w_query, lambda_head, head_gain, w_out, rotated_key_cache, value_cache, lengths
):
    seqs, features = tokens.shape
    heads = lambda_head.shape[0]
    positions = rotated_key_cache.shape[1]
    count = lax.axis_size("kv")
    cosine, sine = tables(lengths, LANES // HEAD_FEATURES)
    limits = lengths - lax.axis_index("kv").astype(jnp.int32) * positions
    side = lax.axis_index("tp").astype(jnp.int32).reshape(1)
    signs = jnp.broadcast_to(
        jnp.concatenate([jnp.ones_like(lambda_head), -lambda_head])[:, None], (2 * heads, LANES)
    )

    partial = call(
        project_kernel,
        jax.ShapeDtypeStruct((heads + 1, seqs, LANES), F32),
        [VMEM] * 3,
        flops=2 * seqs * features * heads * LANES,
    )(tokens, norm_gain[None, :], w_query)
    queries = exchanged(partial, "kv")

    blocks = call(
        functools.partial(attend_kernel, features * count, count),
        jax.ShapeDtypeStruct((seqs + 1, 2 * heads, LANES), BF16),
        [SMEM] + [VMEM] * (count + 4),
        [pltpu.VMEM((seqs, heads, LANES), F32)],
        flops=8 * seqs * heads * positions * LANES,
    )(limits, *queries, cosine, sine, rotated_key_cache, value_cache)
    gathered = exchanged(blocks, "kv")

    columns = w_out.shape[1] // 2
    flops = 2 * seqs * heads * VALUE_DIM * columns
    normed, sent = call(
        functools.partial(finish_kernel, count),
        (
            jax.ShapeDtypeStruct((seqs, heads * VALUE_DIM), BF16),
            jax.ShapeDtypeStruct((seqs, columns), F32),
        ),
        [SMEM] + [VMEM] * (count + 3),
        [pltpu.VMEM((seqs, heads, LANES), F32)],
        flops=flops,
    )(side, *gathered, signs, head_gain[None, :], w_out)
    received = lax.ppermute(sent, "tp", [(0, 1), (1, 0)])
    own = call(
        own_kernel, jax.ShapeDtypeStruct((seqs, columns), F32), [SMEM, VMEM, VMEM], flops=flops
    )(side, normed, w_out)
    return (own + received).astype(BF16)


def far_device(
    tokens, norm_gain, w_query, lambda_head, head_gain, w_out, rotated_key_cache, value_cache, lengths
):
    seqs, features = tokens.shape
    heads = lambda_head.shape[0]
    positions = rotated_key_cache.shape[1]
    widened = tokens.astype(F32)
    scaled = (widened * norm_gain).astype(BF16)
    squares = lax.psum(jnp.sum(widened * widened, -1), "kv")
    raw = lax.psum(jnp.dot(scaled, w_query, preferred_element_type=F32), "kv")
    scale = lax.rsqrt(squares / (features * lax.axis_size("kv")) + EPS)
    raw = (raw * scale[:, None]).reshape(seqs, heads, 2, HEAD_FEATURES)
    cosine, sine = tables(lengths, 1)
    turned = jnp.roll(raw, HEAD_FEATURES // 2, -1)
    query = raw * cosine[:, None, None, :] + turned * sine[:, None, None, :]
    keys = rotated_key_cache.reshape(seqs, positions, 2, HEAD_FEATURES)
    scores = jnp.einsum(
        "bhmd,bpmd->bhmp", query, keys, preferred_element_type=F32, precision=lax.Precision.HIGHEST
    ) * HEAD_FEATURES ** (-0.5)
    places = lax.axis_index("kv") * positions + jnp.arange(positions, dtype=jnp.int32)
    valid = (places[None, :] < lengths[:, None])[:, None, None, :]
    masked = jnp.where(valid, scores, MASKED)
    top = lax.pmax(jnp.max(masked, -1), "kv")
    weights = jnp.where(valid, jnp.exp(masked - top[..., None]), 0.0)
    totals = lax.psum(jnp.sum(weights, -1), "kv")
    numerators = lax.psum(
        jnp.einsum("bhmp,bpv->bhmv", weights.astype(BF16), value_cache, preferred_element_type=F32), "kv"
    )
    averaged = numerators / totals[..., None]
    head_out = averaged[..., 0, :] - lambda_head[None, :, None] * averaged[..., 1, :]
    factor = lax.rsqrt(jnp.mean(head_out * head_out, -1, keepdims=True) + EPS)
    normed = (head_out * factor * head_gain).astype(BF16).reshape(seqs, heads * VALUE_DIM)
    projected = jnp.dot(normed, w_out, preferred_element_type=F32)
    return lax.psum_scatter(projected, "tp", scatter_dimension=1, tiled=True).astype(BF16)


def solution(mesh):
    count = mesh.shape["kv"]
    near = count <= 4 and count & (count - 1) == 0 and mesh.shape["tp"] == 2
    in_specs = (
        P("dp", "kv"),
        P("kv"),
        P("kv", "tp"),
        P("tp"),
        P(),
        P("tp", "kv"),
        P("dp", "kv", None),
        P("dp", "kv", None),
        P("dp"),
    )
    return jax.shard_map(
        near_device if near else far_device,
        mesh=mesh,
        in_specs=in_specs,
        out_specs=P("dp", ("kv", "tp")),
        check_vma=False,
    )
```

```python
import functools

import jax
import jax.numpy as jnp
from jax import lax
from jax.experimental import pallas as pl
from jax.experimental.pallas import tpu as pltpu
from jax.sharding import PartitionSpec as P


HEAD_FEATURES = 64
VALUE_DIM = 128
LANES = 128
EPS = 1e-05
ROPE_BASE = 10000.0
MASKED = -1e30
F32 = jnp.float32
BF16 = jnp.bfloat16
GRANT = 16 << 20
CHUNKS = 4
VMEM = pl.BlockSpec(memory_space=pltpu.VMEM)
SMEM = pl.BlockSpec(memory_space=pltpu.SMEM)
HBM = pl.BlockSpec(memory_space=pltpu.HBM)


def lane_index(shape):
    return lax.broadcasted_iota(jnp.int32, shape, len(shape) - 1)


def split3(x):
    high = x.astype(BF16).astype(F32)
    rest = x - high
    middle = rest.astype(BF16).astype(F32)
    return high, middle, (rest - middle).astype(BF16).astype(F32)


def project_kernel(tokens_hbm, gain_hbm, weights_hbm, out_ref, tokens_ref, gain_ref, weights_ref, done):
    heads = out_ref.shape[0] - 1
    features = weights_ref.shape[0]
    rows = features // CHUNKS
    copies = [
        pltpu.make_async_copy(tokens_hbm, tokens_ref, done.at[CHUNKS]),
        pltpu.make_async_copy(gain_hbm, gain_ref, done.at[CHUNKS + 1]),
    ]
    for chunk in range(CHUNKS):
        here = pl.ds(chunk * rows, rows)
        copies.append(pltpu.make_async_copy(weights_hbm.at[here], weights_ref.at[here], done.at[chunk]))
    for copy in copies:
        copy.start()
    copies[0].wait()
    copies[1].wait()
    widened = tokens_ref[...].astype(F32)
    squares = jnp.sum(widened * widened, -1, keepdims=True)
    scaled = (widened * gain_ref[...]).astype(BF16)
    part = None
    for chunk in range(CHUNKS):
        here = slice(chunk * rows, (chunk + 1) * rows)
        copies[2 + chunk].wait()
        product = jnp.dot(scaled[:, here], weights_ref[here], preferred_element_type=F32)
        part = product if part is None else part + product
    for head in range(heads):
        out_ref[head] = part[:, head * LANES : (head + 1) * LANES]
    out_ref[heads] = jnp.broadcast_to(squares, out_ref.shape[1:])


def stage(sources, targets, done, meanwhile=None):
    copies = [
        pltpu.make_async_copy(source, target, done.at[i])
        for i, (source, target) in enumerate(zip(sources, targets))
    ]
    for copy in copies:
        copy.start()
    if meanwhile is not None:
        meanwhile()
    for copy in copies:
        copy.wait()


def stage_cache_kernel(lengths_ref, first_ref, keys_hbm, values_hbm, limits_ref, keys_ref, values_ref, done):
    def limits():
        row = lax.broadcasted_iota(jnp.int32, limits_ref.shape, 0)
        value = jnp.zeros(limits_ref.shape, jnp.int32)
        for seq in range(limits_ref.shape[0]):
            value = jnp.where(row == seq, lengths_ref[seq] - first_ref[0], value)
        limits_ref[...] = value

    stage((keys_hbm, values_hbm), (keys_ref, values_ref), done, limits)


def stage_output_kernel(lambda_ref, weights_hbm, signs_ref, weights_ref, done):
    def signs():
        heads = signs_ref.shape[0] // 2
        row = lax.broadcasted_iota(jnp.int32, signs_ref.shape, 0)
        value = jnp.ones(signs_ref.shape, F32)
        for head in range(heads):
            value = jnp.where(row == heads + head, -lambda_ref[head], value)
        signs_ref[...] = value

    stage((weights_hbm,), (weights_ref,), done, signs)


def attend_kernel(width, count, limits_ref, *refs):
    parts, (cosine_ref, sine_ref, keys_ref, values_ref, out_ref, query_ref) = refs[:count], refs[count:]
    heads = parts[0].shape[0] - 1
    seqs, positions = keys_ref.shape[:2]

    def summed(index):
        total = parts[0][index]
        for part in parts[1:]:
            total = total + part[index]
        return total

    scale = lax.rsqrt(summed(heads) / width + EPS) * HEAD_FEATURES ** (-0.5)
    cosine, sine = cosine_ref[...] * scale, sine_ref[...] * scale
    half = HEAD_FEATURES // 2
    low = (lane_index(cosine.shape) % HEAD_FEATURES) < half
    for head in range(heads):
        raw = summed(head)
        turned = jnp.where(low, pltpu.roll(raw, LANES - half, 1), pltpu.roll(raw, half, 1))
        query_ref[:, head, :] = raw * cosine + turned * sine

    first = lane_index((heads, LANES)) < HEAD_FEATURES
    rows = 2 * heads
    lanes = lane_index((rows, LANES))
    places = lane_index((rows, positions))
    maxima = jnp.zeros((rows, LANES), F32)
    totals = jnp.zeros((rows, LANES), F32)
    for seq in range(seqs):
        pieces = split3(query_ref[seq])
        left = jnp.concatenate(
            [jnp.where(keep, piece, 0.0) for piece in pieces for keep in (first, ~first)], 0
        ).astype(BF16)
        products = lax.dot_general(
            left, keys_ref[seq], (((1,), (1,)), ((), ())), preferred_element_type=F32
        )
        scores = products[:rows] + (products[rows : 2 * rows] + products[2 * rows :])
        valid = places < limits_ref[seq : seq + 1, :1]
        masked = jnp.where(valid, scores, MASKED)
        top = jnp.max(masked, -1, keepdims=True)
        weights = jnp.where(valid, jnp.exp(masked - top), 0.0)
        maxima = jnp.where(lanes == seq, top, maxima)
        totals = jnp.where(lanes == seq, jnp.sum(weights, -1, keepdims=True), totals)
        out_ref[seq] = jnp.dot(
            weights.astype(BF16), values_ref[seq], preferred_element_type=F32
        ).astype(BF16)
    packed = jnp.zeros((rows, LANES), F32)
    for place, piece in enumerate(split3(maxima) + split3(totals)):
        inside = (lanes >= place * seqs) & (lanes < (place + 1) * seqs)
        moved = pltpu.roll(piece, place * seqs, 1) if place else piece
        packed = jnp.where(inside, moved, packed)
    out_ref[seqs] = packed.astype(BF16)


def combine(parts, signs_ref, gain_ref, mixed_ref):
    seqs, rows = parts[0].shape[0] - 1, parts[0].shape[1]
    heads = rows // 2

    def unpacked(part, place):
        packed = part[seqs].astype(F32)
        total = None
        for piece in range(place, place + 3):
            moved = pltpu.roll(packed, LANES - piece * seqs, 1) if piece else packed
            total = moved if total is None else total + moved
        return total

    maxima = [unpacked(part, 0) for part in parts]
    top = functools.reduce(jnp.maximum, maxima)
    factors = [jnp.exp(own - top) for own in maxima]
    totals = sum(factor * unpacked(part, 3) for factor, part in zip(factors, parts))
    shares = signs_ref[...] / totals
    factors = [factor * shares for factor in factors]
    gain = gain_ref[...]
    for seq in range(seqs):
        both = sum(
            factor[:, seq : seq + 1] * part[seq].astype(F32) for factor, part in zip(factors, parts)
        )
        head_out = both[:heads] + both[heads:]
        mean = jnp.mean(head_out * head_out, -1, keepdims=True)
        mixed_ref[seq] = head_out * lax.rsqrt(mean + EPS) * gain


def finish_kernel(count, side_ref, *refs):
    parts = refs[:count]
    signs_ref, gain_ref, weights_ref, normed_ref, sent_ref, mixed_ref = refs[count:]
    combine(parts, signs_ref, gain_ref, mixed_ref)
    for head in range(mixed_ref.shape[1]):
        normed_ref[:, head * VALUE_DIM : (head + 1) * VALUE_DIM] = mixed_ref[:, head, :].astype(BF16)
    width = sent_ref.shape[1]
    start = pl.multiple_of((1 - side_ref[0]) * width, width)
    sent_ref[...] = jnp.dot(
        normed_ref[...], weights_ref[:, pl.ds(start, width)], preferred_element_type=F32
    )


def own_kernel(side_ref, normed_ref, weights_ref, out_ref):
    width = out_ref.shape[1]
    start = pl.multiple_of(side_ref[0] * width, width)
    out_ref[...] = jnp.dot(
        normed_ref[...], weights_ref[:, pl.ds(start, width)], preferred_element_type=F32
    )


def call(kernel, out_shape, in_specs, scratch=(), flops=0):
    out_specs = jax.tree.map(lambda _: VMEM, out_shape)
    return pl.pallas_call(
        kernel,
        out_shape=out_shape,
        in_specs=in_specs,
        out_specs=out_specs,
        scratch_shapes=scratch,
        compiler_params=pltpu.CompilerParams(vmem_limit_bytes=GRANT),
        cost_estimate=pl.CostEstimate(flops=flops, bytes_accessed=1 << 20, transcendentals=0),
    )


def in_hbm(*arrays):
    return tuple(pltpu.with_memory_space_constraint(x, pltpu.HBM) for x in arrays)


def like(*arrays):
    return tuple(jax.ShapeDtypeStruct(x.shape, x.dtype) for x in arrays)


def exchanged(x, axis):
    count = lax.axis_size(axis)
    received = []
    for step in range(count - 1, 0, -1):
        pairs = [(source, source ^ step) for source in range(count)]
        received.append(lax.ppermute(x, axis, pairs))
    return [x] + received


def tables(lengths, copies):
    half = HEAD_FEATURES // 2
    frequency = 1.0 / ROPE_BASE ** (jnp.arange(half, dtype=F32) / half)
    angles = (lengths - 1).astype(F32)[:, None] * frequency[None, :]
    cosine, sine = jnp.cos(angles), jnp.sin(angles)
    return (
        jnp.concatenate([cosine, cosine] * copies, -1),
        jnp.concatenate([-sine, sine] * copies, -1),
    )


def near_device(
    tokens, norm_gain, w_query, lambda_head, head_gain, w_out, rotated_key_cache, value_cache, lengths
):
    seqs, features = tokens.shape
    heads = lambda_head.shape[0]
    positions = rotated_key_cache.shape[1]
    count = lax.axis_size("kv")
    cosine, sine = tables(lengths, LANES // HEAD_FEATURES)
    first = (lax.axis_index("kv").astype(jnp.int32) * positions).reshape(1)
    side = lax.axis_index("tp").astype(jnp.int32).reshape(1)

    partial = call(
        project_kernel,
        jax.ShapeDtypeStruct((heads + 1, seqs, LANES), F32),
        [HBM] * 3,
        [
            pltpu.VMEM((seqs, features), BF16),
            pltpu.VMEM((1, features), F32),
            pltpu.VMEM(w_query.shape, BF16),
            pltpu.SemaphoreType.DMA((CHUNKS + 2,)),
        ],
        flops=2 * seqs * features * heads * LANES,
    )(*in_hbm(tokens, norm_gain[None, :], w_query))
    queries = exchanged(partial, "kv")
    limits, keys, values = call(
        stage_cache_kernel,
        (jax.ShapeDtypeStruct((seqs, LANES), jnp.int32), *like(rotated_key_cache, value_cache)),
        [SMEM, SMEM, HBM, HBM],
        [pltpu.SemaphoreType.DMA((2,))],
        flops=1 << 20,
    )(lengths, first, *in_hbm(rotated_key_cache, value_cache))

    blocks = call(
        functools.partial(attend_kernel, features * count, count),
        jax.ShapeDtypeStruct((seqs + 1, 2 * heads, LANES), BF16),
        [VMEM] * (count + 5),
        [pltpu.VMEM((seqs, heads, LANES), F32)],
        flops=8 * seqs * heads * positions * LANES,
    )(limits, *queries, cosine, sine, keys, values)
    gathered = exchanged(blocks, "kv")
    signs, weights = call(
        stage_output_kernel,
        (jax.ShapeDtypeStruct((2 * heads, LANES), F32), *like(w_out)),
        [SMEM, HBM],
        [pltpu.SemaphoreType.DMA((1,))],
        flops=1 << 20,
    )(lambda_head, *in_hbm(w_out))

    columns = w_out.shape[1] // 2
    flops = 2 * seqs * heads * VALUE_DIM * columns
    normed, sent = call(
        functools.partial(finish_kernel, count),
        (
            jax.ShapeDtypeStruct((seqs, heads * VALUE_DIM), BF16),
            jax.ShapeDtypeStruct((seqs, columns), F32),
        ),
        [SMEM] + [VMEM] * (count + 3),
        [pltpu.VMEM((seqs, heads, LANES), F32)],
        flops=flops,
    )(side, *gathered, signs, head_gain[None, :], weights)
    received = lax.ppermute(sent, "tp", [(0, 1), (1, 0)])
    own = call(
        own_kernel, jax.ShapeDtypeStruct((seqs, columns), F32), [SMEM, VMEM, VMEM], flops=flops
    )(side, normed, weights)
    return (own + received).astype(BF16)


def far_device(
    tokens, norm_gain, w_query, lambda_head, head_gain, w_out, rotated_key_cache, value_cache, lengths
):
    seqs, features = tokens.shape
    heads = lambda_head.shape[0]
    positions = rotated_key_cache.shape[1]
    widened = tokens.astype(F32)
    scaled = (widened * norm_gain).astype(BF16)
    squares = lax.psum(jnp.sum(widened * widened, -1), "kv")
    raw = lax.psum(jnp.dot(scaled, w_query, preferred_element_type=F32), "kv")
    scale = lax.rsqrt(squares / (features * lax.axis_size("kv")) + EPS)
    raw = (raw * scale[:, None]).reshape(seqs, heads, 2, HEAD_FEATURES)
    cosine, sine = tables(lengths, 1)
    turned = jnp.roll(raw, HEAD_FEATURES // 2, -1)
    query = raw * cosine[:, None, None, :] + turned * sine[:, None, None, :]
    keys = rotated_key_cache.reshape(seqs, positions, 2, HEAD_FEATURES)
    scores = jnp.einsum(
        "bhmd,bpmd->bhmp", query, keys, preferred_element_type=F32, precision=lax.Precision.HIGHEST
    ) * HEAD_FEATURES ** (-0.5)
    places = lax.axis_index("kv") * positions + jnp.arange(positions, dtype=jnp.int32)
    valid = (places[None, :] < lengths[:, None])[:, None, None, :]
    masked = jnp.where(valid, scores, MASKED)
    top = lax.pmax(jnp.max(masked, -1), "kv")
    weights = jnp.where(valid, jnp.exp(masked - top[..., None]), 0.0)
    totals = lax.psum(jnp.sum(weights, -1), "kv")
    numerators = lax.psum(
        jnp.einsum("bhmp,bpv->bhmv", weights.astype(BF16), value_cache, preferred_element_type=F32), "kv"
    )
    averaged = numerators / totals[..., None]
    head_out = averaged[..., 0, :] - lambda_head[None, :, None] * averaged[..., 1, :]
    factor = lax.rsqrt(jnp.mean(head_out * head_out, -1, keepdims=True) + EPS)
    normed = (head_out * factor * head_gain).astype(BF16).reshape(seqs, heads * VALUE_DIM)
    projected = jnp.dot(normed, w_out, preferred_element_type=F32)
    return lax.psum_scatter(projected, "tp", scatter_dimension=1, tiled=True).astype(BF16)


def solution(mesh):
    count = mesh.shape["kv"]
    near = count <= 4 and count & (count - 1) == 0 and mesh.shape["tp"] == 2
    in_specs = (
        P("dp", "kv"),
        P("kv"),
        P("kv", "tp"),
        P("tp"),
        P(),
        P("tp", "kv"),
        P("dp", "kv", None),
        P("dp", "kv", None),
        P("dp"),
    )
    return jax.shard_map(
        near_device if near else far_device,
        mesh=mesh,
        in_specs=in_specs,
        out_specs=P("dp", ("kv", "tp")),
        check_vma=False,
    )
```

```python
import functools

import jax
import jax.numpy as jnp
from jax import lax
from jax.experimental import pallas as pl
from jax.experimental.pallas import tpu as pltpu
from jax.sharding import PartitionSpec as P


HEAD_FEATURES = 64
VALUE_DIM = 128
LANES = 128
EPS = 1e-05
ROPE_BASE = 10000.0
MASKED = -1e30
F32 = jnp.float32
BF16 = jnp.bfloat16
GRANT = 16 << 20
CHUNKS = 4
VMEM = pl.BlockSpec(memory_space=pltpu.VMEM)
SMEM = pl.BlockSpec(memory_space=pltpu.SMEM)
HBM = pl.BlockSpec(memory_space=pltpu.HBM)


def lane_index(shape):
    return lax.broadcasted_iota(jnp.int32, shape, len(shape) - 1)


def split3(x):
    high = x.astype(BF16).astype(F32)
    rest = x - high
    middle = rest.astype(BF16).astype(F32)
    return high, middle, (rest - middle).astype(BF16).astype(F32)


def project_kernel(tokens_hbm, gain_hbm, weights_hbm, out_ref, tokens_ref, gain_ref, weights_ref, done):
    heads = out_ref.shape[0] - 1
    features = weights_ref.shape[0]
    rows = features // CHUNKS
    copies = [
        pltpu.make_async_copy(tokens_hbm, tokens_ref, done.at[CHUNKS]),
        pltpu.make_async_copy(gain_hbm, gain_ref, done.at[CHUNKS + 1]),
    ]
    for chunk in range(CHUNKS):
        here = pl.ds(chunk * rows, rows)
        copies.append(pltpu.make_async_copy(weights_hbm.at[here], weights_ref.at[here], done.at[chunk]))
    for copy in copies:
        copy.start()
    copies[0].wait()
    copies[1].wait()
    widened = tokens_ref[...].astype(F32)
    squares = jnp.sum(widened * widened, -1, keepdims=True)
    scaled = (widened * gain_ref[...]).astype(BF16)
    part = None
    for chunk in range(CHUNKS):
        here = slice(chunk * rows, (chunk + 1) * rows)
        copies[2 + chunk].wait()
        product = jnp.dot(scaled[:, here], weights_ref[here], preferred_element_type=F32)
        part = product if part is None else part + product
    for head in range(heads):
        out_ref[head] = part[:, head * LANES : (head + 1) * LANES]
    out_ref[heads] = jnp.broadcast_to(squares, out_ref.shape[1:])


def stage(sources, targets, done, meanwhile=None):
    copies = [
        pltpu.make_async_copy(source, target, done.at[i])
        for i, (source, target) in enumerate(zip(sources, targets))
    ]
    for copy in copies:
        copy.start()
    if meanwhile is not None:
        meanwhile()
    for copy in copies:
        copy.wait()


def stage_cache_kernel(lengths_ref, first_ref, keys_hbm, values_hbm, limits_ref, keys_ref, values_ref, done):
    def limits():
        row = lax.broadcasted_iota(jnp.int32, limits_ref.shape, 0)
        value = jnp.zeros(limits_ref.shape, jnp.int32)
        for seq in range(limits_ref.shape[0]):
            value = jnp.where(row == seq, lengths_ref[seq] - first_ref[0], value)
        limits_ref[...] = value

    stage((keys_hbm, values_hbm), (keys_ref, values_ref), done, limits)


def stage_output_kernel(lambda_ref, weights_hbm, signs_ref, weights_ref, done):
    def signs():
        heads = signs_ref.shape[0] // 2
        row = lax.broadcasted_iota(jnp.int32, signs_ref.shape, 0)
        value = jnp.ones(signs_ref.shape, F32)
        for head in range(heads):
            value = jnp.where(row == heads + head, -lambda_ref[head], value)
        signs_ref[...] = value

    stage((weights_hbm,), (weights_ref,), done, signs)


def attend_kernel(width, count, limits_ref, *refs):
    parts, (cosine_ref, sine_ref, keys_ref, values_ref, out_ref, query_ref) = refs[:count], refs[count:]
    heads = parts[0].shape[0] - 1
    seqs, positions = keys_ref.shape[:2]

    def summed(index):
        total = parts[0][index]
        for part in parts[1:]:
            total = total + part[index]
        return total

    scale = lax.rsqrt(summed(heads) / width + EPS) * HEAD_FEATURES ** (-0.5)
    cosine, sine = cosine_ref[...] * scale, sine_ref[...] * scale
    half = HEAD_FEATURES // 2
    low = (lane_index(cosine.shape) % HEAD_FEATURES) < half
    for head in range(heads):
        raw = summed(head)
        turned = jnp.where(low, pltpu.roll(raw, LANES - half, 1), pltpu.roll(raw, half, 1))
        query_ref[:, head, :] = raw * cosine + turned * sine

    first = lane_index((heads, LANES)) < HEAD_FEATURES
    rows = 2 * heads
    lanes = lane_index((rows, LANES))
    places = lane_index((rows, positions))
    maxima = jnp.zeros((rows, LANES), F32)
    totals = jnp.zeros((rows, LANES), F32)
    scores = []
    for seq in range(seqs):
        pieces = split3(query_ref[seq])
        left = jnp.concatenate(
            [jnp.where(keep, piece, 0.0) for piece in pieces for keep in (first, ~first)], 0
        ).astype(BF16)
        products = lax.dot_general(
            left, keys_ref[seq], (((1,), (1,)), ((), ())), preferred_element_type=F32
        )
        scores.append(products[:rows] + (products[rows : 2 * rows] + products[2 * rows :]))
    weights = []
    for seq in range(seqs):
        valid = places < limits_ref[seq : seq + 1, :1]
        masked = jnp.where(valid, scores[seq], MASKED)
        top = jnp.max(masked, -1, keepdims=True)
        weight = jnp.where(valid, jnp.exp(masked - top), 0.0)
        maxima = jnp.where(lanes == seq, top, maxima)
        totals = jnp.where(lanes == seq, jnp.sum(weight, -1, keepdims=True), totals)
        weights.append(weight.astype(BF16))
    numerators = [
        jnp.dot(weights[seq], values_ref[seq], preferred_element_type=F32) for seq in range(seqs)
    ]
    for seq in range(seqs):
        out_ref[seq] = numerators[seq].astype(BF16)
    packed = jnp.zeros((rows, LANES), F32)
    for place, piece in enumerate(split3(maxima) + split3(totals)):
        inside = (lanes >= place * seqs) & (lanes < (place + 1) * seqs)
        moved = pltpu.roll(piece, place * seqs, 1) if place else piece
        packed = jnp.where(inside, moved, packed)
    out_ref[seqs] = packed.astype(BF16)


def combine(parts, signs_ref, gain_ref, mixed_ref):
    seqs, rows = parts[0].shape[0] - 1, parts[0].shape[1]
    heads = rows // 2

    def unpacked(part, place):
        packed = part[seqs].astype(F32)
        total = None
        for piece in range(place, place + 3):
            moved = pltpu.roll(packed, LANES - piece * seqs, 1) if piece else packed
            total = moved if total is None else total + moved
        return total

    maxima = [unpacked(part, 0) for part in parts]
    top = functools.reduce(jnp.maximum, maxima)
    factors = [jnp.exp(own - top) for own in maxima]
    totals = sum(factor * unpacked(part, 3) for factor, part in zip(factors, parts))
    shares = signs_ref[...] / totals
    factors = [factor * shares for factor in factors]
    gain = gain_ref[...]
    for seq in range(seqs):
        both = sum(
            factor[:, seq : seq + 1] * part[seq].astype(F32) for factor, part in zip(factors, parts)
        )
        head_out = both[:heads] + both[heads:]
        mean = jnp.mean(head_out * head_out, -1, keepdims=True)
        mixed_ref[seq] = head_out * lax.rsqrt(mean + EPS) * gain


def finish_kernel(count, side_ref, *refs):
    parts = refs[:count]
    signs_ref, gain_ref, weights_ref, normed_ref, sent_ref, mixed_ref = refs[count:]
    combine(parts, signs_ref, gain_ref, mixed_ref)
    for head in range(mixed_ref.shape[1]):
        normed_ref[:, head * VALUE_DIM : (head + 1) * VALUE_DIM] = mixed_ref[:, head, :].astype(BF16)
    width = sent_ref.shape[1]
    start = pl.multiple_of((1 - side_ref[0]) * width, width)
    sent_ref[...] = jnp.dot(
        normed_ref[...], weights_ref[:, pl.ds(start, width)], preferred_element_type=F32
    )


def own_kernel(side_ref, normed_ref, weights_ref, out_ref):
    width = out_ref.shape[1]
    start = pl.multiple_of(side_ref[0] * width, width)
    out_ref[...] = jnp.dot(
        normed_ref[...], weights_ref[:, pl.ds(start, width)], preferred_element_type=F32
    )


def call(kernel, out_shape, in_specs, scratch=(), flops=0):
    out_specs = jax.tree.map(lambda _: VMEM, out_shape)
    return pl.pallas_call(
        kernel,
        out_shape=out_shape,
        in_specs=in_specs,
        out_specs=out_specs,
        scratch_shapes=scratch,
        compiler_params=pltpu.CompilerParams(vmem_limit_bytes=GRANT),
        cost_estimate=pl.CostEstimate(flops=flops, bytes_accessed=1 << 20, transcendentals=0),
    )


def in_hbm(*arrays):
    return tuple(pltpu.with_memory_space_constraint(x, pltpu.HBM) for x in arrays)


def like(*arrays):
    return tuple(jax.ShapeDtypeStruct(x.shape, x.dtype) for x in arrays)


def exchanged(x, axis):
    count = lax.axis_size(axis)
    received = []
    for step in range(count - 1, 0, -1):
        pairs = [(source, source ^ step) for source in range(count)]
        received.append(lax.ppermute(x, axis, pairs))
    return [x] + received


def tables(lengths, copies):
    half = HEAD_FEATURES // 2
    frequency = 1.0 / ROPE_BASE ** (jnp.arange(half, dtype=F32) / half)
    angles = (lengths - 1).astype(F32)[:, None] * frequency[None, :]
    cosine, sine = jnp.cos(angles), jnp.sin(angles)
    return (
        jnp.concatenate([cosine, cosine] * copies, -1),
        jnp.concatenate([-sine, sine] * copies, -1),
    )


def near_device(
    tokens, norm_gain, w_query, lambda_head, head_gain, w_out, rotated_key_cache, value_cache, lengths
):
    seqs, features = tokens.shape
    heads = lambda_head.shape[0]
    positions = rotated_key_cache.shape[1]
    count = lax.axis_size("kv")
    cosine, sine = tables(lengths, LANES // HEAD_FEATURES)
    first = (lax.axis_index("kv").astype(jnp.int32) * positions).reshape(1)
    side = lax.axis_index("tp").astype(jnp.int32).reshape(1)

    partial = call(
        project_kernel,
        jax.ShapeDtypeStruct((heads + 1, seqs, LANES), F32),
        [HBM] * 3,
        [
            pltpu.VMEM((seqs, features), BF16),
            pltpu.VMEM((1, features), F32),
            pltpu.VMEM(w_query.shape, BF16),
            pltpu.SemaphoreType.DMA((CHUNKS + 2,)),
        ],
        flops=2 * seqs * features * heads * LANES,
    )(*in_hbm(tokens, norm_gain[None, :], w_query))
    queries = exchanged(partial, "kv")
    limits, keys, values = call(
        stage_cache_kernel,
        (jax.ShapeDtypeStruct((seqs, LANES), jnp.int32), *like(rotated_key_cache, value_cache)),
        [SMEM, SMEM, HBM, HBM],
        [pltpu.SemaphoreType.DMA((2,))],
        flops=1 << 20,
    )(lengths, first, *in_hbm(rotated_key_cache, value_cache))

    blocks = call(
        functools.partial(attend_kernel, features * count, count),
        jax.ShapeDtypeStruct((seqs + 1, 2 * heads, LANES), BF16),
        [VMEM] * (count + 5),
        [pltpu.VMEM((seqs, heads, LANES), F32)],
        flops=8 * seqs * heads * positions * LANES,
    )(limits, *queries, cosine, sine, keys, values)
    gathered = exchanged(blocks, "kv")
    signs, weights = call(
        stage_output_kernel,
        (jax.ShapeDtypeStruct((2 * heads, LANES), F32), *like(w_out)),
        [SMEM, HBM],
        [pltpu.SemaphoreType.DMA((1,))],
        flops=1 << 20,
    )(lambda_head, *in_hbm(w_out))

    columns = w_out.shape[1] // 2
    flops = 2 * seqs * heads * VALUE_DIM * columns
    normed, sent = call(
        functools.partial(finish_kernel, count),
        (
            jax.ShapeDtypeStruct((seqs, heads * VALUE_DIM), BF16),
            jax.ShapeDtypeStruct((seqs, columns), F32),
        ),
        [SMEM] + [VMEM] * (count + 3),
        [pltpu.VMEM((seqs, heads, LANES), F32)],
        flops=flops,
    )(side, *gathered, signs, head_gain[None, :], weights)
    received = lax.ppermute(sent, "tp", [(0, 1), (1, 0)])
    own = call(
        own_kernel, jax.ShapeDtypeStruct((seqs, columns), F32), [SMEM, VMEM, VMEM], flops=flops
    )(side, normed, weights)
    return (own + received).astype(BF16)


def far_device(
    tokens, norm_gain, w_query, lambda_head, head_gain, w_out, rotated_key_cache, value_cache, lengths
):
    seqs, features = tokens.shape
    heads = lambda_head.shape[0]
    positions = rotated_key_cache.shape[1]
    widened = tokens.astype(F32)
    scaled = (widened * norm_gain).astype(BF16)
    squares = lax.psum(jnp.sum(widened * widened, -1), "kv")
    raw = lax.psum(jnp.dot(scaled, w_query, preferred_element_type=F32), "kv")
    scale = lax.rsqrt(squares / (features * lax.axis_size("kv")) + EPS)
    raw = (raw * scale[:, None]).reshape(seqs, heads, 2, HEAD_FEATURES)
    cosine, sine = tables(lengths, 1)
    turned = jnp.roll(raw, HEAD_FEATURES // 2, -1)
    query = raw * cosine[:, None, None, :] + turned * sine[:, None, None, :]
    keys = rotated_key_cache.reshape(seqs, positions, 2, HEAD_FEATURES)
    scores = jnp.einsum(
        "bhmd,bpmd->bhmp", query, keys, preferred_element_type=F32, precision=lax.Precision.HIGHEST
    ) * HEAD_FEATURES ** (-0.5)
    places = lax.axis_index("kv") * positions + jnp.arange(positions, dtype=jnp.int32)
    valid = (places[None, :] < lengths[:, None])[:, None, None, :]
    masked = jnp.where(valid, scores, MASKED)
    top = lax.pmax(jnp.max(masked, -1), "kv")
    weights = jnp.where(valid, jnp.exp(masked - top[..., None]), 0.0)
    totals = lax.psum(jnp.sum(weights, -1), "kv")
    numerators = lax.psum(
        jnp.einsum("bhmp,bpv->bhmv", weights.astype(BF16), value_cache, preferred_element_type=F32), "kv"
    )
    averaged = numerators / totals[..., None]
    head_out = averaged[..., 0, :] - lambda_head[None, :, None] * averaged[..., 1, :]
    factor = lax.rsqrt(jnp.mean(head_out * head_out, -1, keepdims=True) + EPS)
    normed = (head_out * factor * head_gain).astype(BF16).reshape(seqs, heads * VALUE_DIM)
    projected = jnp.dot(normed, w_out, preferred_element_type=F32)
    return lax.psum_scatter(projected, "tp", scatter_dimension=1, tiled=True).astype(BF16)


def solution(mesh):
    count = mesh.shape["kv"]
    near = count <= 4 and count & (count - 1) == 0 and mesh.shape["tp"] == 2
    in_specs = (
        P("dp", "kv"),
        P("kv"),
        P("kv", "tp"),
        P("tp"),
        P(),
        P("tp", "kv"),
        P("dp", "kv", None),
        P("dp", "kv", None),
        P("dp"),
    )
    return jax.shard_map(
        near_device if near else far_device,
        mesh=mesh,
        in_specs=in_specs,
        out_specs=P("dp", ("kv", "tp")),
        check_vma=False,
    )
```
